32 devices in a mesh: rep: 2 (over x), fs: 8 (over z, y), tp: 2 (over core).
Axes of the slice: x: 2, y: 2, z: 4, core: 2. Of those that a mesh axis runs over, the one named last changes fastest.
Arguments:
- hidden_in: bfloat16 [10240, 2048], P(('rep', 'fs'), 'tp'), may hold values from -6 to 6
- mix_gain: float32 [2048], replicated, may hold values from 0.1 to 1.9
- w_value: bfloat16 [2048, 1024], P('fs', 'tp'), may hold values from -0.125 to 0.125
- w_gate: bfloat16 [2048, 1024], P('fs', 'tp'), may hold values from -0.125 to 0.125
- conv_taps: float32 [31, 1024], P(None, 'tp'), may hold values from -5 to 5
- conv_bias: float32 [1024], P('tp'), may hold values from -3 to 3
- chan_gain: float32 [1024], P('tp'), may hold values from 0.1 to 1.9
- chan_bias: float32 [1024], P('tp'), may hold values from -3 to 3
- w_back: bfloat16 [1024, 2048], P('tp', 'fs'), may hold values from -0.1875 to 0.1875
- feed_gain: float32 [2048], replicated, may hold values from 0.1 to 1.9
- w_up: bfloat16 [2048, 8192], P(None, ('fs', 'tp')), may hold values from -0.125 to 0.125
- w_down: bfloat16 [8192, 2048], P(('fs', 'tp')), may hold values from -0.0625 to 0.0625
Outputs:
- layer_out: bfloat16 [10240, 2048], P(('rep', 'fs'), 'tp')
The draws below stay inside these ranges and needn't reach their ends.
All inputs are finite; a program needn't handle non-finite values.
Results may differ from the reference program's by a relative error of at most 0.015.
Values may be sent and summed in bfloat16 or wider, within the bound.
A program may use at most 128 MiB of HBM per device.

```python
import jax
import jax.numpy as jnp
from jax import lax

D = 2048
CH = 1024
FF = 8192
KW = 31
LEN = 128
TOKENS = 10240
N_FS = 8
N_TP = 2


def draw_conv_taps(key, part):
    entry_key, rough_key = jax.random.split(jax.random.fold_in(key, 11))
    channel_ramp = jnp.arange(CH, dtype=jnp.float32) / CH
    roughness = jax.random.uniform(rough_key, (KW, CH), jnp.float32, 0.5, 1.5)
    entries = jnp.clip(jax.random.normal(entry_key, (KW, CH), jnp.float32), -4.0, 4.0)
    growth = 3.0 ** channel_ramp
    return (entries * roughness * growth[None, :] * KW ** (-0.5)).astype(jnp.float32)


def shard_levels(own_key, dims, cuts, least, high):
    loudness, own = 1.0, jax.random.fold_in(own_key, 6)
    for dim, blocks in cuts:
        heights = jnp.exp(jax.random.uniform(jax.random.fold_in(own, dim), (blocks,), jnp.float32, least / len(cuts), high / len(cuts)))
        loudness = loudness * jnp.repeat(heights, dims[dim] // blocks).reshape([-1 if axis == dim else 1 for axis in range(len(dims))])
    return loudness


def gaussian(own_key, extent, deviation, most, cuts=(), kind=jnp.bfloat16):
    values = deviation * jax.random.normal(own_key, extent, jnp.float32)
    if cuts:
        values = values * shard_levels(own_key, extent, cuts, -0.22, 0.18)
    return jnp.clip(values, -most, most).astype(kind)


def setup_inputs(seed: int = 0) -> dict:
    key_of = jax.random.split(jax.random.key(seed), 13)
    hidden_in = gaussian(key_of[0], (TOKENS, D), 1.0, 6.0, ((0, 16), (1, 2)))
    mix_gain = jnp.clip(1.0 + 0.18 * jax.random.normal(key_of[1], (D,), jnp.float32), 0.1, 1.9)
    w_value = gaussian(key_of[2], (D, CH), D ** -0.5, 0.125, ((0, 8), (1, 2)))
    w_gate = gaussian(key_of[3], (D, CH), D ** -0.5, 0.125, ((0, 8), (1, 2)))
    conv_taps = draw_conv_taps(jax.random.fold_in(key_of[12], 71), 0)
    conv_bias = gaussian(key_of[5], (CH,), 0.5, 3.0, ((0, 2),), jnp.float32)
    chan_gain = jnp.clip(1.0 + 0.18 * jax.random.normal(key_of[6], (CH,), jnp.float32), 0.1, 1.9)
    chan_bias = gaussian(key_of[7], (CH,), 0.5, 3.0, ((0, 2),), jnp.float32)
    w_back = gaussian(key_of[8], (CH, D), CH ** -0.5, 0.1875, ((0, 2), (1, 8)))
    feed_gain = jnp.clip(1.0 + 0.18 * jax.random.normal(key_of[9], (D,), jnp.float32), 0.1, 1.9)
    w_up = gaussian(key_of[10], (D, FF), D ** -0.5, 0.125, ((1, 16),))
    w_down = gaussian(key_of[11], (FF, D), FF ** -0.5, 0.0625, ((0, 16),))
    return dict(hidden_in=hidden_in, mix_gain=mix_gain, w_value=w_value, w_gate=w_gate, conv_taps=conv_taps, conv_bias=conv_bias, chan_gain=chan_gain, chan_bias=chan_bias, w_back=w_back, feed_gain=feed_gain, w_up=w_up, w_down=w_down)


def rms_norm(stream, gain):
    values = stream.astype(jnp.float32)
    scaled = values * lax.rsqrt(lax.optimization_barrier(jnp.mean(values * values, axis=-1, keepdims=True)) + 1e-06)
    return (scaled * gain).astype(jnp.bfloat16)

def causal_filter(gated, conv_taps, conv_bias):
    channels = gated.shape[1]
    blocks = gated.reshape(gated.shape[0] // LEN, LEN, channels)
    padded = jnp.pad(blocks, ((0, 0), (KW - 1, 0), (0, 0)))
    result = jnp.zeros_like(blocks) + conv_bias
    for tap_index in range(KW):
        result = result + conv_taps[tap_index] * padded[:, tap_index:tap_index + LEN]
    return result.reshape(gated.shape)

def blocked_sum(left, right):
    inner = left.shape[1] // N_TP
    running = jnp.zeros((left.shape[0], right.shape[1]), jnp.float32)
    for block_index in range(N_TP):
        partial_value = jnp.dot(left[:, block_index * inner:(block_index + 1) * inner], right[block_index * inner:(block_index + 1) * inner], preferred_element_type=jnp.float32)
        running = running + partial_value.astype(jnp.bfloat16).astype(jnp.float32)
    return running

def strided_sum(left, right):
    rows = left.shape[0]
    width = right.shape[1]
    block = left.shape[1] // (N_FS * N_TP)
    left_blocks = left.reshape(rows, N_FS, N_TP, block)
    right_blocks = right.reshape(N_FS, N_TP, block, width)
    running = jnp.zeros((rows, width), jnp.float32)
    for block_index in range(N_TP):
        partial_value = jnp.dot(left_blocks[:, :, block_index].reshape(rows, N_FS * block), right_blocks[:, block_index].reshape(N_FS * block, width), preferred_element_type=jnp.float32)
        running = running + partial_value.astype(jnp.bfloat16).astype(jnp.float32)
    return running

def reference(hidden_in, mix_gain, w_value, w_gate, conv_taps, conv_bias, chan_gain, chan_bias, w_back, feed_gain, w_up, w_down):
    normed = rms_norm(hidden_in, mix_gain)
    value_proj = jnp.dot(normed, w_value, preferred_element_type=jnp.float32)
    gate_proj = jnp.dot(normed, w_gate, preferred_element_type=jnp.float32)
    gated = value_proj * jax.nn.sigmoid(gate_proj)
    filtered = causal_filter(gated, conv_taps, conv_bias)
    chan_mean = lax.optimization_barrier(jnp.mean(filtered, axis=1, keepdims=True))
    chan_var = lax.optimization_barrier(jnp.mean(filtered * filtered, axis=1, keepdims=True)) - chan_mean * chan_mean
    centred = (filtered - chan_mean) * lax.rsqrt(chan_var + 1e-05) * chan_gain + chan_bias
    mixer_act = jax.nn.silu(centred).astype(jnp.bfloat16)
    mixed = blocked_sum(mixer_act, w_back)
    second = (hidden_in.astype(jnp.float32) + mixed).astype(jnp.bfloat16)
    normed_feed = rms_norm(second, feed_gain)
    up_proj = jnp.dot(normed_feed, w_up, preferred_element_type=jnp.float32)
    hidden = jnp.square(jax.nn.relu(up_proj)).astype(jnp.bfloat16)
    feed = strided_sum(hidden, w_down)
    return (second.astype(jnp.float32) + feed).astype(jnp.bfloat16)
```

```python
import jax
import jax.numpy as jnp
from jax import lax
from jax.sharding import Mesh, PartitionSpec as P

KW = 31
LEN = 128


SWAP = [(0, 1), (1, 0)]


def swap(value, axis):
    return lax.ppermute(value, axis, SWAP)


def joined(own, other, index, axis):
    return jnp.where(
        index == 0,
        jnp.concatenate([own, other], axis=axis),
        jnp.concatenate([other, own], axis=axis),
    )


def rms_norm(stream, gain):
    values = stream.astype(jnp.float32)
    scaled = values * lax.rsqrt(jnp.mean(values * values, axis=-1, keepdims=True) + 1e-06)
    return (scaled * gain).astype(jnp.bfloat16)


def causal_filter(gated, conv_taps, conv_bias):
    channels = gated.shape[1]
    blocks = gated.reshape(gated.shape[0] // LEN, LEN, channels)
    padded = jnp.pad(blocks, ((0, 0), (KW - 1, 0), (0, 0)))
    result = jnp.zeros_like(blocks) + conv_bias
    for tap_index in range(KW):
        result = result + conv_taps[tap_index] * padded[:, tap_index : tap_index + LEN]
    return result.reshape(gated.shape)


def plane_slots(piece):
    half = piece.shape[0] // 2
    from_rep = swap(piece, "rep")
    from_fy = swap(piece, "fy")
    diag_low = swap(from_rep[:half], "fy")
    diag_high = swap(from_fy[half:], "rep")
    return [piece, from_rep, from_fy, jnp.concatenate([diag_low, diag_high], axis=0)]


def full_features(slot, tp_index):
    return joined(slot, swap(slot, "tp"), tp_index, 1)


def halves(partial, tp_index):
    width = partial.shape[1] // 2
    own = lax.dynamic_slice_in_dim(partial, tp_index * width, width, 1)
    other = lax.dynamic_slice_in_dim(partial, (1 - tp_index) * width, width, 1)
    return own, other


def tp_reduced(partial, tp_index):
    own, other = halves(partial, tp_index)
    return own.astype(jnp.float32) + swap(other, "tp").astype(jnp.float32)


def plane_reduced(compute):
    half = None
    diag = compute(3)
    half = diag.shape[0] // 2
    via_rep = swap(diag[:half].astype(jnp.bfloat16), "rep").astype(jnp.float32)
    via_fy = swap(diag[half:].astype(jnp.bfloat16), "fy").astype(jnp.float32)
    for_rep = compute(1)
    for_rep = jnp.concatenate([for_rep[:half], for_rep[half:] + via_fy], axis=0)
    from_rep = swap(for_rep.astype(jnp.bfloat16), "rep")
    for_fy = compute(2)
    for_fy = jnp.concatenate([for_fy[:half] + via_rep, for_fy[half:]], axis=0)
    from_fy = swap(for_fy.astype(jnp.bfloat16), "fy")
    return compute(0) + from_rep.astype(jnp.float32) + from_fy.astype(jnp.float32)


def shards(
    hidden_in,
    mix_gain,
    w_value,
    w_gate,
    conv_taps,
    conv_bias,
    chan_gain,
    chan_bias,
    w_back,
    feed_gain,
    w_up,
    w_down,
):
    rep, fy, tp = lax.axis_index("rep"), lax.axis_index("fy"), lax.axis_index("tp")
    n_fz = lax.axis_size("fz")
    n_rep, n_fy, n_tp = lax.axis_size("rep"), lax.axis_size("fy"), lax.axis_size("tp")
    parts = n_rep * n_fy
    mine, theirs = rep * n_fy + fy, rep * n_fy + 1 - fy
    rows = w_value.shape[0]
    own_ch = w_value.shape[1] // parts

    def columns(array, which):
        return lax.dynamic_slice_in_dim(array, which * own_ch, own_ch, array.ndim - 1)

    def front_pack(which):
        packed_in = jnp.concatenate([columns(w_value, which), columns(w_gate, which)], axis=1)
        packed_out = lax.dynamic_slice_in_dim(w_back, which * own_ch, own_ch, 0)
        return jnp.concatenate(
            [packed_in.reshape(-1, own_ch), packed_out.reshape(-1, own_ch)], axis=0
        )

    kept, sent = front_pack(mine), front_pack(theirs)
    received = swap(sent, "fy")
    pair = joined(kept[None], received[None], fy, 0)
    front = lax.all_gather(pair, "fz", axis=0, tiled=True)
    in_rows = rows * 2
    w_in = front[:, :in_rows].reshape(n_fz * n_fy * rows, 2 * own_ch)
    back_cols = w_back.shape[1]
    whole_back = (
        front[:, in_rows:]
        .reshape(n_fz * n_fy, own_ch, back_cols)
        .transpose(1, 0, 2)
        .reshape(own_ch, n_fz * n_fy * back_cols)
    )

    own_ff = w_up.shape[1] // n_rep
    up = lax.all_gather(
        lax.dynamic_slice_in_dim(w_up, rep * own_ff, own_ff, 1), "fz", axis=1, tiled=True
    )
    down = lax.all_gather(
        lax.dynamic_slice_in_dim(w_down, rep * own_ff, own_ff, 0), "fz", axis=0, tiled=True
    )

    taps, bias = columns(conv_taps, mine), columns(conv_bias, mine)
    gain, shift = columns(chan_gain, mine), columns(chan_bias, mine)

    slots = plane_slots(hidden_in)
    tokens = hidden_in.shape[0]
    filtered = []
    for slot in slots:
        normed = rms_norm(full_features(slot, tp), mix_gain)
        both = jnp.dot(normed, w_in, preferred_element_type=jnp.float32)
        gated = both[:, :own_ch] * jax.nn.sigmoid(both[:, own_ch:])
        filtered.append(causal_filter(gated, taps, bias))
    stats = jnp.stack(
        [jnp.stack([jnp.sum(f, axis=1), jnp.sum(f * f, axis=1)]) for f in filtered]
    )
    stats = stats + swap(stats, "tp")
    other = swap(stats, "rep")
    stats = stats + jnp.stack([other[1], other[0], other[3], other[2]])
    other = swap(stats, "fy")
    stats = stats + jnp.stack([other[2], other[3], other[0], other[1]])
    channel_total = own_ch * parts * n_tp
    acts = []
    for index in range(4):
        chan_mean = (stats[index, 0] / channel_total)[:, None]
        chan_var = (stats[index, 1] / channel_total)[:, None] - chan_mean * chan_mean
        centred = (filtered[index] - chan_mean) * lax.rsqrt(chan_var + 1e-05) * gain + shift
        acts.append(jax.nn.silu(centred).astype(jnp.bfloat16))

    def mixed_share(index):
        partial = jnp.dot(acts[index], whole_back, preferred_element_type=jnp.float32)
        return tp_reduced(partial.astype(jnp.bfloat16), tp)

    mixed = plane_reduced(mixed_share)
    second = (hidden_in.astype(jnp.float32) + mixed).astype(jnp.bfloat16)

    feeds = [rms_norm(full_features(slot, tp), feed_gain) for slot in plane_slots(second)]

    def feed_share(index):
        up_proj = jnp.dot(feeds[index], up, preferred_element_type=jnp.float32)
        hidden = jnp.square(jax.nn.relu(up_proj)).astype(jnp.bfloat16)
        partial = jnp.dot(hidden, down, preferred_element_type=jnp.float32)
        return tp_reduced(partial.astype(jnp.bfloat16), tp)

    feed = plane_reduced(feed_share)
    return (second.astype(jnp.float32) + feed).astype(jnp.bfloat16)


def solution(mesh):
    n_rep, n_fs, n_tp = mesh.shape["rep"], mesh.shape["fs"], mesh.shape["tp"]
    split = Mesh(mesh.devices.reshape(n_rep, n_fs // 2, 2, n_tp), ("rep", "fz", "fy", "tp"))
    fs = ("fz", "fy")
    rows = P(("rep", "fz", "fy"), "tp")
    placed = (
        rows,
        P(),
        P(fs, "tp"),
        P(fs, "tp"),
        P(None, "tp"),
        P("tp"),
        P("tp"),
        P("tp"),
        P("tp", fs),
        P(),
        P(None, ("fz", "fy", "tp")),
        P(("fz", "fy", "tp"), None),
    )
    return jax.shard_map(shards, mesh=split, in_specs=placed, out_specs=rows, check_vma=False)
```

```python
import jax
import jax.numpy as jnp
from jax import lax
from jax.sharding import Mesh, PartitionSpec as P


KW = 31
LEN = 128


SWAP = [(0, 1), (1, 0)]


def swap(value, axis):
    return lax.ppermute(value, axis, SWAP)


def ordered(own, other, index, axis):
    first = jnp.where(index == 0, own, other)
    return jnp.concatenate([first, jnp.where(index == 0, other, own)], axis=axis)


def own_first(array, index, axis):
    half = array.shape[axis] // 2
    return jnp.concatenate(
        [
            lax.dynamic_slice_in_dim(array, index * half, half, axis),
            lax.dynamic_slice_in_dim(array, (1 - index) * half, half, axis),
        ],
        axis=axis,
    )


def rms_norm(stream, gain):
    values = stream.astype(jnp.float32)
    scaled = values * lax.rsqrt(jnp.mean(values * values, axis=-1, keepdims=True) + 1e-06)
    return (scaled * gain).astype(jnp.bfloat16)


def causal_filter(gated, conv_taps, conv_bias):
    channels = gated.shape[1]
    blocks = gated.reshape(gated.shape[0] // LEN, LEN, channels)
    padded = jnp.pad(blocks, ((0, 0), (KW - 1, 0), (0, 0)))
    result = jnp.zeros_like(blocks) + conv_bias
    for tap_index in range(KW):
        result = result + conv_taps[tap_index] * padded[:, tap_index : tap_index + LEN]
    return result.reshape(gated.shape)


def plane_slots(piece):
    half = piece.shape[0] // 2
    from_rep = swap(piece, "rep")
    from_fy = swap(piece, "fy")
    diag_low = swap(from_rep[:half], "fy")
    diag_high = swap(from_fy[half:], "rep")
    return [piece, from_rep, from_fy, jnp.concatenate([diag_low, diag_high], axis=0)]


def full_features(slot):
    return jnp.concatenate([slot, swap(slot, "tp")], axis=1)


def tp_reduced(left, right):
    width = right.shape[1] // 2
    sent = jnp.dot(left, right[:, width:], preferred_element_type=jnp.float32)
    kept = jnp.dot(left, right[:, :width], preferred_element_type=jnp.float32)
    return kept + swap(sent.astype(jnp.bfloat16), "tp").astype(jnp.float32)


def plane_reduced(compute):
    diag = compute(3)
    half = diag.shape[0] // 2
    via_rep = swap(diag[:half].astype(jnp.bfloat16), "rep").astype(jnp.float32)
    via_fy = swap(diag[half:].astype(jnp.bfloat16), "fy").astype(jnp.float32)
    for_rep = compute(1)
    for_rep = jnp.concatenate([for_rep[:half], for_rep[half:] + via_fy], axis=0)
    from_rep = swap(for_rep.astype(jnp.bfloat16), "rep")
    for_fy = compute(2)
    for_fy = jnp.concatenate([for_fy[:half] + via_rep, for_fy[half:]], axis=0)
    from_fy = swap(for_fy.astype(jnp.bfloat16), "fy")
    return compute(0) + from_rep.astype(jnp.float32) + from_fy.astype(jnp.float32)


def block(
    hidden_in,
    mix_gain,
    w_value,
    w_gate,
    conv_taps,
    conv_bias,
    chan_gain,
    chan_bias,
    w_back,
    feed_gain,
    w_up,
    w_down,
):
    rep, fy, tp = lax.axis_index("rep"), lax.axis_index("fy"), lax.axis_index("tp")
    n_fz = lax.axis_size("fz")
    n_rep, n_fy, n_tp = lax.axis_size("rep"), lax.axis_size("fy"), lax.axis_size("tp")
    parts = n_rep * n_fy
    mine, theirs = rep * n_fy + fy, rep * n_fy + 1 - fy
    rows, back_cols = w_value.shape[0], w_back.shape[1]
    own_ch = w_value.shape[1] // parts

    def columns(array, which):
        return lax.dynamic_slice_in_dim(array, which * own_ch, own_ch, array.ndim - 1)

    def front_pack(which):
        packed_out = lax.dynamic_slice_in_dim(w_back, which * own_ch, own_ch, 0)
        pieces = [packed_out]
        if back_cols > own_ch:
            pieces = [
                packed_out[:, at : at + own_ch] for at in range(0, back_cols, own_ch)
            ]
        elif back_cols < own_ch:
            pieces = [packed_out.reshape(-1, own_ch)]
        return jnp.concatenate([columns(w_value, which), columns(w_gate, which)] + pieces, axis=0)

    received = swap(front_pack(theirs), "fy")
    slots = plane_slots(hidden_in)
    pair = ordered(front_pack(mine)[None], received[None], fy, 0)
    front = lax.all_gather(pair, "fz", axis=0, tiled=True)
    blocks = n_fz * n_fy
    w_in = own_first(
        jnp.concatenate(
            [
                front[:, :rows].reshape(blocks * rows, own_ch),
                front[:, rows : 2 * rows].reshape(blocks * rows, own_ch),
            ],
            axis=1,
        ),
        tp,
        0,
    )
    if back_cols >= own_ch:
        whole_back = front[:, 2 * rows :].reshape(blocks * (back_cols // own_ch), own_ch, own_ch)
    else:
        whole_back = front[:, 2 * rows :].reshape(blocks, own_ch, back_cols)
    whole_back = own_first(
        whole_back.transpose(1, 0, 2).reshape(own_ch, blocks * back_cols), tp, 1
    )

    own_ff = w_up.shape[1] // n_rep
    up_part = own_first(lax.dynamic_slice_in_dim(w_up, rep * own_ff, own_ff, 1), tp, 0)
    down_part = own_first(lax.dynamic_slice_in_dim(w_down, rep * own_ff, own_ff, 0), tp, 1)
    up = lax.all_gather(up_part, "fz", axis=1, tiled=True)
    down = lax.all_gather(down_part, "fz", axis=0, tiled=True)

    taps, bias = columns(conv_taps, mine), columns(conv_bias, mine)
    gain, shift = columns(chan_gain, mine), columns(chan_bias, mine)

    tokens = hidden_in.shape[0]
    mix_rolled, feed_rolled = own_first(mix_gain, tp, 0), own_first(feed_gain, tp, 0)
    gated = []
    for slot in slots:
        normed = rms_norm(full_features(slot), mix_rolled)
        both = jnp.dot(normed, w_in, preferred_element_type=jnp.float32)
        gated.append(both[:, :own_ch] * jax.nn.sigmoid(both[:, own_ch:]))
    filtered = causal_filter(jnp.concatenate(gated, axis=0), taps, bias)
    stats = jnp.stack([jnp.sum(filtered, axis=1), jnp.sum(filtered * filtered, axis=1)])
    stats = stats.reshape(2, 4, tokens)
    stats = stats + swap(stats, "tp")
    other = swap(stats, "rep")
    stats = stats + jnp.stack([other[:, at] for at in (1, 0, 3, 2)], axis=1)
    other = swap(stats, "fy")
    stats = stats + jnp.stack([other[:, at] for at in (2, 3, 0, 1)], axis=1)
    stats = stats.reshape(2, 4 * tokens) / (own_ch * parts * n_tp)
    chan_mean = stats[0][:, None]
    chan_var = stats[1][:, None] - chan_mean * chan_mean
    centred = (filtered - chan_mean) * lax.rsqrt(chan_var + 1e-05) * gain + shift
    act = jax.nn.silu(centred).astype(jnp.bfloat16)

    def mixed_share(index):
        return tp_reduced(act[index * tokens : (index + 1) * tokens], whole_back)

    mixed = plane_reduced(mixed_share)
    second = (hidden_in.astype(jnp.float32) + mixed).astype(jnp.bfloat16)

    hidden = []
    for slot in plane_slots(second):
        normed = rms_norm(full_features(slot), feed_rolled)
        up_proj = jnp.dot(normed, up, preferred_element_type=jnp.float32)
        hidden.append(jnp.square(jax.nn.relu(up_proj)).astype(jnp.bfloat16))
    hidden = list(lax.optimization_barrier(tuple(hidden)))

    def feed_share(index):
        return tp_reduced(hidden[index], down)

    feed = plane_reduced(feed_share)
    return (second.astype(jnp.float32) + feed).astype(jnp.bfloat16)


def solution(mesh):
    n_rep, n_fs, n_tp = mesh.shape["rep"], mesh.shape["fs"], mesh.shape["tp"]
    split = Mesh(mesh.devices.reshape(n_rep, n_fs // 2, 2, n_tp), ("rep", "fz", "fy", "tp"))
    fs = ("fz", "fy")
    rows = P(("rep", "fz", "fy"), "tp")
    placed = (
        rows,
        P(),
        P(fs, "tp"),
        P(fs, "tp"),
        P(None, "tp"),
        P("tp"),
        P("tp"),
        P("tp"),
        P("tp", fs),
        P(),
        P(None, ("fz", "fy", "tp")),
        P(("fz", "fy", "tp"), None),
    )
    return jax.shard_map(block, mesh=split, in_specs=placed, out_specs=rows, check_vma=False)
```

```python
import jax
import jax.numpy as jnp
from jax import lax
from jax.sharding import Mesh, PartitionSpec as P


KW = 31
LEN = 128


SWAP = [(0, 1), (1, 0)]


def swap(value, axis):
    return lax.ppermute(value, axis, SWAP)


def ordered(own, other, index, axis):
    first = jnp.where(index == 0, own, other)
    return jnp.concatenate([first, jnp.where(index == 0, other, own)], axis=axis)


def own_first(array, index, axis):
    half = array.shape[axis] // 2
    return jnp.concatenate(
        [
            lax.dynamic_slice_in_dim(array, index * half, half, axis),
            lax.dynamic_slice_in_dim(array, (1 - index) * half, half, axis),
        ],
        axis=axis,
    )


def rms_norm(stream, gain):
    values = stream.astype(jnp.float32)
    scaled = values * lax.rsqrt(jnp.mean(values * values, axis=-1, keepdims=True) + 1e-06)
    return (scaled * gain).astype(jnp.bfloat16)


def causal_filter(gated, conv_taps, conv_bias):
    channels = gated.shape[1]
    blocks = gated.reshape(gated.shape[0] // LEN, LEN, channels)
    padded = jnp.pad(blocks, ((0, 0), (KW - 1, 0), (0, 0)))
    result = jnp.zeros_like(blocks) + conv_bias
    for tap_index in range(KW):
        result = result + conv_taps[tap_index] * padded[:, tap_index : tap_index + LEN]
    return result.reshape(gated.shape)


def plane_slots(piece):
    half = piece.shape[0] // 2
    low, high = piece[:half], piece[half:]
    rep_low, fy_high = swap(low, "rep"), swap(high, "fy")
    rep_high, fy_low = swap(high, "rep"), swap(low, "fy")
    diag_low, diag_high = swap(rep_low, "fy"), swap(fy_high, "rep")
    return [
        piece,
        jnp.concatenate([rep_low, rep_high], axis=0),
        jnp.concatenate([fy_low, fy_high], axis=0),
        jnp.concatenate([diag_low, diag_high], axis=0),
    ]


def full_features(slot):
    return jnp.concatenate([slot, swap(slot, "tp")], axis=1)


def tp_reduced(left, right):
    width = right.shape[1] // 2
    sent = jnp.dot(left, right[:, width:], preferred_element_type=jnp.float32)
    kept = jnp.dot(left, right[:, :width], preferred_element_type=jnp.float32)
    return kept + swap(sent.astype(jnp.bfloat16), "tp").astype(jnp.float32)


def plane_reduced(compute):
    diag = compute(3)
    half = diag.shape[0] // 2
    via_rep = swap(diag[:half].astype(jnp.bfloat16), "rep").astype(jnp.float32)
    via_fy = swap(diag[half:].astype(jnp.bfloat16), "fy").astype(jnp.float32)
    for_rep, for_fy = compute(1), compute(2)
    rep_low = swap(for_rep[:half].astype(jnp.bfloat16), "rep")
    fy_high = swap(for_fy[half:].astype(jnp.bfloat16), "fy")
    rep_high = swap((for_rep[half:] + via_fy).astype(jnp.bfloat16), "rep")
    fy_low = swap((for_fy[:half] + via_rep).astype(jnp.bfloat16), "fy")
    from_rep = jnp.concatenate([rep_low, rep_high], axis=0).astype(jnp.float32)
    from_fy = jnp.concatenate([fy_low, fy_high], axis=0).astype(jnp.float32)
    return compute(0) + from_rep + from_fy


def block(
    hidden_in,
    mix_gain,
    w_value,
    w_gate,
    conv_taps,
    conv_bias,
    chan_gain,
    chan_bias,
    w_back,
    feed_gain,
    w_up,
    w_down,
):
    rep, fy, tp = lax.axis_index("rep"), lax.axis_index("fy"), lax.axis_index("tp")
    n_fz = lax.axis_size("fz")
    n_rep, n_fy, n_tp = lax.axis_size("rep"), lax.axis_size("fy"), lax.axis_size("tp")
    parts = n_rep * n_fy
    mine, theirs = rep * n_fy + fy, rep * n_fy + 1 - fy
    rows, back_cols = w_value.shape[0], w_back.shape[1]
    own_ch = w_value.shape[1] // parts

    def columns(array, which):
        return lax.dynamic_slice_in_dim(array, which * own_ch, own_ch, array.ndim - 1)

    def front_pack(which):
        packed_out = lax.dynamic_slice_in_dim(w_back, which * own_ch, own_ch, 0)
        pieces = [packed_out]
        if back_cols > own_ch:
            pieces = [
                packed_out[:, at : at + own_ch] for at in range(0, back_cols, own_ch)
            ]
        elif back_cols < own_ch:
            pieces = [packed_out.reshape(-1, own_ch)]
        return jnp.concatenate([columns(w_value, which), columns(w_gate, which)] + pieces, axis=0)

    received = swap(front_pack(theirs), "fy")
    slots = plane_slots(hidden_in)
    pair = ordered(front_pack(mine)[None], received[None], fy, 0)
    fz = lax.axis_index("fz")
    front = lax.dynamic_update_slice_in_dim(
        jnp.zeros((n_fz * n_fy,) + pair.shape[1:], pair.dtype), pair, fz * n_fy, 0
    )
    for step in range(1, n_fz):
        ring = [(at, (at + step) % n_fz) for at in range(n_fz)]
        arrived = lax.ppermute(pair, "fz", ring)
        front = lax.dynamic_update_slice_in_dim(
            front, arrived, lax.rem(fz + n_fz - step, n_fz) * n_fy, 0
        )
    blocks = n_fz * n_fy
    w_in = own_first(
        jnp.concatenate(
            [
                front[:, :rows].reshape(blocks * rows, own_ch),
                front[:, rows : 2 * rows].reshape(blocks * rows, own_ch),
            ],
            axis=1,
        ),
        tp,
        0,
    )
    if back_cols >= own_ch:
        whole_back = front[:, 2 * rows :].reshape(blocks * (back_cols // own_ch), own_ch, own_ch)
    else:
        whole_back = front[:, 2 * rows :].reshape(blocks, own_ch, back_cols)
    whole_back = own_first(
        whole_back.transpose(1, 0, 2).reshape(own_ch, blocks * back_cols), tp, 1
    )

    own_ff = w_up.shape[1] // n_rep
    up_part = own_first(lax.dynamic_slice_in_dim(w_up, rep * own_ff, own_ff, 1), tp, 0)
    down_part = own_first(lax.dynamic_slice_in_dim(w_down, rep * own_ff, own_ff, 0), tp, 1)
    up = lax.all_gather(up_part, "fz", axis=1, tiled=True)
    down = lax.all_gather(down_part, "fz", axis=0, tiled=True)

    taps, bias = columns(conv_taps, mine), columns(conv_bias, mine)
    gain, shift = columns(chan_gain, mine), columns(chan_bias, mine)

    tokens = hidden_in.shape[0]
    mix_rolled, feed_rolled = own_first(mix_gain, tp, 0), own_first(feed_gain, tp, 0)
    gated = []
    for slot in slots:
        normed = rms_norm(full_features(slot), mix_rolled)
        both = jnp.dot(normed, w_in, preferred_element_type=jnp.float32)
        gated.append(both[:, :own_ch] * jax.nn.sigmoid(both[:, own_ch:]))
    filtered = causal_filter(jnp.concatenate(gated, axis=0), taps, bias)
    stats = jnp.stack([jnp.sum(filtered, axis=1), jnp.sum(filtered * filtered, axis=1)])
    stats = stats.reshape(2, 4, tokens)
    stats = stats + swap(stats, "tp")
    other = swap(stats, "rep")
    stats = stats + jnp.stack([other[:, at] for at in (1, 0, 3, 2)], axis=1)
    other = swap(stats, "fy")
    stats = stats + jnp.stack([other[:, at] for at in (2, 3, 0, 1)], axis=1)
    stats = stats.reshape(2, 4 * tokens) / (own_ch * parts * n_tp)
    chan_mean = stats[0][:, None]
    chan_var = stats[1][:, None] - chan_mean * chan_mean
    centred = (filtered - chan_mean) * lax.rsqrt(chan_var + 1e-05) * gain + shift
    act = jax.nn.silu(centred).astype(jnp.bfloat16)

    def mixed_share(index):
        return tp_reduced(act[index * tokens : (index + 1) * tokens], whole_back)

    mixed = plane_reduced(mixed_share)
    second = (hidden_in.astype(jnp.float32) + mixed).astype(jnp.bfloat16)

    hidden = []
    for slot in plane_slots(second):
        normed = rms_norm(full_features(slot), feed_rolled)
        up_proj = jnp.dot(normed, up, preferred_element_type=jnp.float32)
        hidden.append(jnp.square(jax.nn.relu(up_proj)).astype(jnp.bfloat16))
    hidden = list(lax.optimization_barrier(tuple(hidden)))

    def feed_share(index):
        return tp_reduced(hidden[index], down)

    feed = plane_reduced(feed_share)
    return (second.astype(jnp.float32) + feed).astype(jnp.bfloat16)


def solution(mesh):
    n_rep, n_fs, n_tp = mesh.shape["rep"], mesh.shape["fs"], mesh.shape["tp"]
    split = Mesh(mesh.devices.reshape(n_rep, n_fs // 2, 2, n_tp), ("rep", "fz", "fy", "tp"))
    fs = ("fz", "fy")
    rows = P(("rep", "fz", "fy"), "tp")
    placed = (
        rows,
        P(),
        P(fs, "tp"),
        P(fs, "tp"),
        P(None, "tp"),
        P("tp"),
        P("tp"),
        P("tp"),
        P("tp", fs),
        P(),
        P(None, ("fz", "fy", "tp")),
        P(("fz", "fy", "tp"), None),
    )
    return jax.shard_map(block, mesh=split, in_specs=placed, out_specs=rows, check_vma=False)
```
